32 devices in a mesh: dp: 4 (over y, x), kv: 4 (over z), tp: 2 (over core).
Axes of the slice: x: 2, y: 2, z: 4, core: 2. Of those that a mesh axis runs over, the one named last changes fastest.
Arguments:
- tokens: bfloat16 [16, 4, 2048], P('dp', None, ('kv', 'tp')), may hold values from -6 to 6
- lengths: int32 [16], P('dp'), may hold values from 1 to 4, 24 in all
- carried: float32 [16, 16, 128, 128], P(('dp', 'kv'), 'tp'), may hold values from -4 to 4
- norm_mix: float32 [2048], replicated, may hold values from 0.1 to 1.9
- w_query: bfloat16 [2048, 16, 128], P(None, 'tp', 'kv'), may hold values from -0.125 to 0.125
- w_forget: bfloat16 [2048, 16, 128], P(None, 'tp', 'kv'), may hold values from -0.125 to 0.125
- w_input: bfloat16 [2048, 16, 128], P(None, 'tp', 'kv'), may hold values from -0.125 to 0.125
- w_gate: bfloat16 [2048, 16, 128], P(None, 'tp', 'kv'), may hold values from -0.125 to 0.125
- lower_bound: float32 [16, 128], P('tp'), may hold values from 0.3 to 0.9
- head_gain: float32 [128], replicated, may hold values from 0.1 to 1.9
- w_out: bfloat16 [16, 128, 2048], P('tp', None, 'kv'), may hold values from -0.125 to 0.125
- mixer_norm_gain: float32 [2048], replicated, may hold values from 0.1 to 1.9
- w_up: bfloat16 [2048, 8192], P(None, ('kv', 'tp')), may hold values from -0.125 to 0.125
- w_down: bfloat16 [8192, 2048], P(('kv', 'tp')), may hold values from -0.09375 to 0.09375
Outputs:
- result: bfloat16 [16, 4, 2048], P('dp', None, ('kv', 'tp'))
- new_state: float32 [16, 16, 128, 128], P(('dp', 'kv'), 'tp')
The draws below stay inside these ranges and needn't reach their ends.
Inputs may be any that keep to these rules, and one draw needn't show every extreme that they name: `lengths`: each sequence's number of live new token slots; some sequence has exactly 4.
All inputs are finite; a program needn't handle non-finite values. No bound on the sum of `lengths` on one device may be relied on, other than what follows from the above.
Results may differ from the reference program's by a relative error of at most 0.013.
Values may be sent and summed in bfloat16 or wider, within the bound.
A program may use at most 64 MiB of HBM per device.

```python
import math
import jax
import jax.numpy as jnp
import numpy as np
from jax import lax

D = 2048
HEADS = 16
HEAD_CHANNELS = 128
FF = 8192
NEW = 4
SEQS = 16


def strengthened(values, key, source, target, parts, factor):
    def block_of(axis_at):
        return (jnp.arange(values.shape[axis_at]) // (values.shape[axis_at] // parts)).reshape((-1,) + (1,) * (values.ndim - 1 - axis_at))

    first = jax.random.permutation(key, parts)[block_of(target)]
    far = (block_of(target) + parts // 2) % parts
    return jnp.where((block_of(source) == first) | (block_of(source) == far), factor * values, values)


def levels(key, shape, cuts, smallest, largest):
    level, own = 1.0, jax.random.fold_in(key, 6)
    for dim, parts in cuts:
        steps = jnp.exp(jax.random.uniform(jax.random.fold_in(own, dim), (parts,), jnp.float32, smallest / len(cuts), largest / len(cuts)))
        level = level * jnp.repeat(steps, shape[dim] // parts).reshape([-1 if axis == dim else 1 for axis in range(len(shape))])
    return level


def profile(amount, total, limit, lean):
    portions = [(1 << 20) // math.isqrt(grade ** lean) + 1 for grade in range(2, amount + 1)]
    spare, counts = total - limit - (amount - 1), [1] * (amount - 1)
    while spare > 0:
        free = [i for i in range(amount - 1) if counts[i] < limit]
        mass, remaining = sum([portions[i] for i in free]), spare
        for i in free:
            addition = min(limit - counts[i], max(1, remaining * portions[i] // mass), spare)
            counts[i] = counts[i] + addition
            spare = spare - addition
    return np.array([limit] + counts)


def ragged(rng, count, total, limit, skew):
    if count == 2:
        one = jax.random.randint(rng, (), max(1, total - limit), min(limit, total - 1) + 1)
        return jnp.stack([one, total - one])
    tallies = jnp.asarray(profile(count, total, limit, skew), jnp.int32)
    twos = (count - 1) // 2
    giver, taker = tallies[1:1 + 2 * twos:2], tallies[2:2 + 2 * twos:2]
    slack = jnp.minimum(giver - 1, limit - taker)
    passed = jax.random.randint(jax.random.fold_in(rng, 1), (twos,), 0, 1 << 20) % (slack + 1)
    tallies = tallies.at[1:1 + 2 * twos:2].set(giver - passed).at[2:2 + 2 * twos:2].set(taker + passed)
    return tallies[jax.random.permutation(jax.random.fold_in(rng, 2), count)]


def centred(own_key, extent, spread, reach, cuts=(), held_as=jnp.bfloat16):
    factor_of = levels(own_key, extent, cuts, -0.22, 0.18) if cuts else 1.0
    entries = jax.random.normal(own_key, extent, jnp.float32) * spread * factor_of
    return jnp.minimum(jnp.maximum(entries, -reach), reach).astype(held_as)


def noise_with(own_key, dims, spread, limit, shards, heavy, dtype=jnp.bfloat16):
    values = spread * jax.random.normal(own_key, dims, jnp.float32)
    if shards:
        values = values * levels(own_key, dims, shards, -0.22, 0.18)
    return jnp.clip(strengthened(values, jax.random.fold_in(own_key, 3), *heavy), -limit, limit).astype(dtype)


def setup_inputs(seed: int = 0) -> dict:
    arg_keys = jax.random.split(jax.random.key(seed), 15)
    tokens = centred(arg_keys[0], (SEQS, NEW, D), 1.0, 6.0, ((0, 4), (2, 8)))
    lengths = ragged(arg_keys[1], SEQS, SEQS + SEQS // 2, NEW, 2).astype(jnp.int32)
    carried = centred(arg_keys[2], (SEQS, HEADS, HEAD_CHANNELS, HEAD_CHANNELS), 0.5, 4.0, ((0, 16), (1, 2)), jnp.float32)
    norm_mix = jnp.clip(1.0 + 0.18 * jax.random.normal(arg_keys[3], (D,), jnp.float32), 0.1, 1.9)
    w_query = centred(arg_keys[4], (D, HEADS, HEAD_CHANNELS), D ** -0.5, 0.125, ((1, 2), (2, 4)))
    w_forget = centred(arg_keys[5], (D, HEADS, HEAD_CHANNELS), D ** -0.5, 0.125, ((1, 2), (2, 4)))
    w_input = centred(arg_keys[6], (D, HEADS, HEAD_CHANNELS), D ** -0.5, 0.125, ((1, 2), (2, 4)))
    w_gate = centred(arg_keys[7], (D, HEADS, HEAD_CHANNELS), D ** -0.5, 0.125, ((1, 2), (2, 4)))
    lower_bound = jnp.clip(0.3 + 0.59999996 * jax.random.uniform(arg_keys[8], (HEADS, HEAD_CHANNELS), jnp.float32) ** levels(arg_keys[8], (HEADS, HEAD_CHANNELS), ((0, 2),), -0.2, 0.2), 0.3, 0.9)
    head_gain = jnp.clip(1.0 + 0.18 * jax.random.normal(arg_keys[9], (HEAD_CHANNELS,), jnp.float32), 0.1, 1.9)
    w_out = centred(arg_keys[10], (HEADS, HEAD_CHANNELS, D), (HEADS * HEAD_CHANNELS) ** -0.5, 0.125, ((0, 2), (2, 4)))
    mixer_norm_gain = jnp.clip(1.0 + 0.18 * jax.random.normal(arg_keys[11], (D,), jnp.float32), 0.1, 1.9)
    w_up = centred(arg_keys[12], (D, FF), D ** -0.5, 0.125, ((1, 8),))
    w_down = noise_with(arg_keys[13], (FF, D), FF ** -0.5, 0.09375, ((0, 8),), (0, 1, 8, 2.0))
    return {"tokens": tokens, "lengths": lengths, "carried": carried, "norm_mix": norm_mix, "w_query": w_query, "w_forget": w_forget, "w_input": w_input, "w_gate": w_gate, "lower_bound": lower_bound, "head_gain": head_gain, "w_out": w_out, "mixer_norm_gain": mixer_norm_gain, "w_up": w_up, "w_down": w_down}


def norm_rows(values, gain):
    floated = values.astype(jnp.float32)
    scaled = floated * lax.rsqrt(lax.optimization_barrier(jnp.mean(floated * floated, axis=-1, keepdims=True)) + 1e-06)
    return (scaled * gain).astype(jnp.bfloat16)

def reference(tokens, lengths, carried, norm_mix, w_query, w_forget, w_input, w_gate, lower_bound, head_gain, w_out, mixer_norm_gain, w_up, w_down):
    normed = norm_rows(tokens, norm_mix).reshape(SEQS * NEW, D)

    def project(weight):
        flat = jnp.dot(normed, weight.reshape(D, HEADS * HEAD_CHANNELS), preferred_element_type=jnp.float32)
        return flat.astype(jnp.bfloat16).reshape(SEQS, NEW, HEADS, HEAD_CHANNELS)
    query_raw = project(w_query)
    forget_raw = project(w_forget)
    value_raw = project(w_input)
    gate_raw = project(w_gate)

    def per_sequence(inputs):
        query_in, forget_in, value_in, gate_in, length, outer_state = inputs
        query_vector = jax.nn.silu(query_in.astype(jnp.float32))
        forget = lower_bound + (1.0 - lower_bound) * jax.nn.sigmoid(forget_in.astype(jnp.float32))
        written = 1.0 - forget
        values = value_in.astype(jnp.float32)
        readouts = []
        for token_position in range(NEW):
            alive = token_position < length
            updated = forget[token_position][:, :, None] * outer_state + written[token_position][:, :, None] * values[token_position][:, None, :]
            outer_state = jnp.where(alive, updated, outer_state)
            state_readout = jnp.einsum('ts,tsz->tz', query_vector[token_position], outer_state, precision=lax.Precision.HIGHEST)
            readouts.append(jnp.where(alive, state_readout, jnp.float32(0.0)))
        state_readout = jnp.stack(readouts)
        scaled = state_readout * lax.rsqrt(lax.optimization_barrier(jnp.mean(state_readout * state_readout, axis=-1, keepdims=True)) + 1e-06)
        gated = scaled * head_gain * jax.nn.silu(gate_in.astype(jnp.float32))
        return (gated.astype(jnp.bfloat16), outer_state)
    mixed, new_state = lax.map(per_sequence, (query_raw, forget_raw, value_raw, gate_raw, lengths, carried))
    branch = jnp.dot(mixed.reshape(SEQS * NEW, HEADS * HEAD_CHANNELS), w_out.reshape(HEADS * HEAD_CHANNELS, D), preferred_element_type=jnp.float32)
    middle = (tokens.reshape(SEQS * NEW, D).astype(jnp.float32) + branch).astype(jnp.bfloat16)
    hidden_in = norm_rows(middle, mixer_norm_gain)
    upward = jnp.dot(hidden_in, w_up, preferred_element_type=jnp.float32)
    activated = jnp.square(jax.nn.relu(upward)).astype(jnp.bfloat16)
    down = jnp.dot(activated, w_down, preferred_element_type=jnp.float32)
    alive_rows = (jnp.arange(NEW)[None, :] < lengths[:, None]).reshape(SEQS * NEW, 1)
    result = jnp.where(alive_rows, middle.astype(jnp.float32) + down, jnp.float32(0.0)).astype(jnp.bfloat16)
    return (result.reshape(SEQS, NEW, D), new_state)
```

```python
import functools

import jax
import jax.numpy as jnp
from jax import lax
from jax.experimental import pallas as pl
from jax.experimental.pallas import tpu as pltpu
from jax.sharding import PartitionSpec as P


def norm_rows(values, gain):
    floated = values.astype(jnp.float32)
    scaled = floated * lax.rsqrt(jnp.mean(floated * floated, axis=-1, keepdims=True) + 1e-06)
    return (scaled * gain).astype(jnp.bfloat16)


def local_collectives(
    tokens,
    lengths,
    carried,
    norm_mix,
    w_query,
    w_forget,
    w_input,
    w_gate,
    lower_bound,
    head_gain,
    w_out,
    mixer_norm_gain,
    w_up,
    w_down,
):
    tp_size = lax.axis_size("tp")
    seq_group, new_rows, piece_width = tokens.shape
    seq_dev = carried.shape[0]
    gathered = lax.all_gather(tokens, ("kv", "tp"), axis=2, tiled=True)
    normed = norm_rows(gathered, norm_mix)
    model_width = gathered.shape[2]

    def project(weight):
        return jnp.einsum(
            "snd,dhk->snhk", normed, weight, preferred_element_type=jnp.float32
        ).astype(jnp.bfloat16)

    query_raw, forget_raw, value_raw, gate_raw = (
        lax.all_to_all(project(w_query), "kv", split_axis=0, concat_axis=3, tiled=True),
        lax.all_to_all(project(w_forget), "kv", split_axis=0, concat_axis=3, tiled=True),
        lax.all_to_all(project(w_input), "kv", split_axis=0, concat_axis=3, tiled=True),
        lax.all_to_all(project(w_gate), "kv", split_axis=0, concat_axis=3, tiled=True),
    )
    own_lengths = lax.dynamic_slice_in_dim(lengths, lax.axis_index("kv") * seq_dev, seq_dev)
    query_vector = jax.nn.silu(query_raw.astype(jnp.float32))
    forget = lower_bound + (1.0 - lower_bound) * jax.nn.sigmoid(forget_raw.astype(jnp.float32))
    written = 1.0 - forget
    values = value_raw.astype(jnp.float32)
    outer_state = carried
    readouts = []
    for token_position in range(new_rows):
        alive = (token_position < own_lengths)[:, None, None, None]
        updated = (
            forget[:, token_position, :, :, None] * outer_state
            + written[:, token_position, :, :, None] * values[:, token_position, :, None, :]
        )
        outer_state = jnp.where(alive, updated, outer_state)
        state_readout = jnp.einsum(
            "shk,shkv->shv",
            query_vector[:, token_position],
            outer_state,
            precision=lax.Precision.HIGHEST,
        )
        readouts.append(jnp.where(alive[..., 0], state_readout, jnp.float32(0.0)))
    state_readout = jnp.stack(readouts, axis=1)
    scaled = state_readout * lax.rsqrt(
        jnp.mean(state_readout * state_readout, axis=-1, keepdims=True) + 1e-06
    )
    mixed = (scaled * head_gain * jax.nn.silu(gate_raw.astype(jnp.float32))).astype(jnp.bfloat16)
    branch = jnp.einsum(
        "snhv,hvd->snd",
        lax.all_gather(mixed, "kv", axis=0, tiled=True),
        w_out,
        preferred_element_type=jnp.float32,
    )
    pair_width = piece_width * tp_size
    summed_total = lax.psum(branch, "tp")
    pair_cols = lax.dynamic_slice_in_dim(gathered, lax.axis_index("kv") * pair_width, pair_width, 2)
    pair_mid = (pair_cols.astype(jnp.float32) + summed_total).astype(jnp.bfloat16)
    full_pair = lax.all_gather(pair_mid, "kv", axis=2, tiled=True)
    middle = lax.dynamic_slice_in_dim(pair_mid, lax.axis_index("tp") * piece_width, piece_width, 2)
    hidden_in = norm_rows(full_pair, mixer_norm_gain).reshape(seq_group * new_rows, model_width)
    upward = jnp.dot(hidden_in, w_up, preferred_element_type=jnp.float32)
    activated = jnp.square(jax.nn.relu(upward)).astype(jnp.bfloat16)
    collected = lax.psum_scatter(
        jnp.einsum("fd,rf->dr", w_down, activated, preferred_element_type=jnp.float32),
        ("kv", "tp"),
        scatter_dimension=0,
        tiled=True,
    )
    down_part = collected.T.reshape(seq_group, new_rows, piece_width)
    alive_rows = (jnp.arange(new_rows)[None, :] < lengths[:, None])[:, :, None]
    result = jnp.where(alive_rows, middle.astype(jnp.float32) + down_part, jnp.float32(0.0)).astype(
        jnp.bfloat16
    )
    return (result, outer_state)


MESH = pl.DeviceIdType.MESH
F32 = jnp.float32
BF16 = jnp.bfloat16


def step_kernel(
    kv_size,
    tp_size,
    tokens,
    lengths,
    carried,
    norm_mix,
    w_query,
    w_forget,
    w_input,
    w_gate,
    lower_bound,
    head_gain,
    w_out,
    mixer_gain,
    w_up,
    w_down,
    result,
    new_state,
    tok_own,
    tok_all,
    lengths_s,
    state_v,
    norm_v,
    w_proj,
    w_turned,
    lower_v,
    head_v,
    w_out_v,
    mixer_v,
    w_up_v,
    w_down_v,
    raw_split,
    swap_src,
    swap_dst,
    by_slot,
    mix_rows,
    mix_src,
    mix_dst,
    mix_wide,
    mid_src,
    mid_dst,
    red_src,
    red_dst,
    load_sem,
    send_tok,
    recv_tok,
    send_out,
    recv_out,
    send_swap,
    recv_swap,
    send_mix,
    recv_mix,
    send_mid,
    recv_mid,
    send_red,
    recv_red,
):
    seqs, slots, piece = tok_own.shape
    group = kv_size * tp_size
    rows = seqs * slots
    heads, chans = lower_v.shape
    width = group * piece
    own_cols = w_proj.shape[1]
    sub = own_cols // heads
    per_tile = chans // sub
    kv = lax.axis_index("kv")
    tp = lax.axis_index("tp")
    me = kv * tp_size + tp
    mate = tp_size - 1 - tp

    mirrored = [kv, kv + 1 - 2 * lax.rem(kv, 2), lax.rem(kv + 2, 4), 3 - kv]

    def along(step):
        return mirrored[step] if kv_size == 4 else lax.rem(kv + step, kv_size)

    def place(column, core):
        return column * tp_size + core, {"kv": column, "tp": core}

    far_peers = [
        place(along(hop), core) for hop in range(kv_size - 1, 0, -1) for core in range(tp_size)
    ]
    far_peers.append(place(kv, mate))
    near_peers = [place(kv, mate)] + [
        place(along(hop), core)
        for hop in range(1, kv_size)
        for core in range(tp_size - 1, -1, -1)
    ]
    far_columns = [place(along(hop), tp) for hop in range(kv_size - 1, 0, -1)]
    near_columns = far_columns[::-1]

    barrier = pltpu.get_barrier_semaphore()
    for _, device in far_peers:
        pl.semaphore_signal(barrier, inc=1, device_id=device, device_id_type=MESH)

    own_out = pl.ds(pl.multiple_of(tp * piece, piece), piece)
    mate_out = pl.ds(pl.multiple_of(mate * piece, piece), piece)
    loads = [
        pltpu.make_async_copy(tokens, tok_own, load_sem.at[0]),
        pltpu.make_async_copy(norm_mix, norm_v, load_sem.at[1]),
        pltpu.make_async_copy(w_query, w_proj.at[0], load_sem.at[2]),
        pltpu.make_async_copy(w_forget, w_proj.at[1], load_sem.at[3]),
        pltpu.make_async_copy(w_input, w_proj.at[2], load_sem.at[4]),
        pltpu.make_async_copy(w_gate, w_proj.at[3], load_sem.at[5]),
        pltpu.make_async_copy(lower_bound, lower_v, load_sem.at[6]),
        pltpu.make_async_copy(head_gain, head_v, load_sem.at[7]),
        pltpu.make_async_copy(carried, state_v, load_sem.at[8]),
        pltpu.make_async_copy(w_out.at[:, own_out], w_out_v.at[tp], load_sem.at[9]),
        pltpu.make_async_copy(mixer_gain, mixer_v, load_sem.at[10]),
        pltpu.make_async_copy(w_up, w_up_v, load_sem.at[11]),
        pltpu.make_async_copy(w_down, w_down_v, load_sem.at[12]),
        pltpu.make_async_copy(lengths, lengths_s, load_sem.at[13]),
    ]
    for index in (0, 2, 3, 4, 5, 1, 6, 7, 13):
        loads[index].start()

    sent = []

    def remote(src, dst, send_sem, recv_sem, device):
        return pltpu.make_async_remote_copy(
            src_ref=src,
            dst_ref=dst,
            send_sem=send_sem,
            recv_sem=recv_sem,
            device_id=device,
            device_id_type=MESH,
        )

    def send(*parts):
        copy = remote(*parts)
        copy.start()
        sent.append(copy)

    def arrived(*parts):
        remote(*parts).wait_recv()

    pl.semaphore_wait(barrier, group - 1)
    loads[0].wait()
    for other, device in far_peers:
        send(tok_own, tok_all.at[me], send_tok.at[other], recv_tok.at[me], device)
    mate_device = place(kv, mate)[1]
    send(w_out.at[:, mate_out], w_out_v.at[tp], send_out.at[0], recv_out.at[0], mate_device)
    for matrix in range(4):
        loads[2 + matrix].wait()
        loads[8 + matrix].start()
        w_turned[:, matrix * own_cols : (matrix + 1) * own_cols] = w_proj[matrix].T
    loads[12].start()
    loads[8].wait()
    state_half = state_v[...].reshape(heads * chans, chans).astype(BF16)
    for index in (1, 6, 7, 13):
        loads[index].wait()

    def stack_rows(block):
        return jnp.concatenate([block[seq].astype(F32) for seq in range(seqs)], axis=0)

    def folded(values):
        total = None
        for at in range(0, piece, chans):
            part = values[:, at : at + chans]
            total = part * part if total is None else total + part * part
        return total

    def span(part):
        return pl.ds(pl.multiple_of(part * piece, piece), piece)

    own_tok = stack_rows(tok_own[...])
    squares = folded(own_tok)
    raw = jnp.dot(
        (own_tok * norm_v[:, span(me)]).astype(BF16),
        w_turned[span(me), :],
        preferred_element_type=F32,
    )
    for other, device in near_peers:
        arrived(tok_own, tok_all.at[other], send_tok.at[other], recv_tok.at[other], device)
        block = stack_rows(tok_all[other])
        squares = squares + folded(block)
        raw = raw + jnp.dot(
            (block * norm_v[:, span(other)]).astype(BF16),
            w_turned[span(other), :],
            preferred_element_type=F32,
        )
    raw = raw * lax.rsqrt(jnp.sum(squares, axis=-1, keepdims=True) / width + 1e-06)
    for matrix in range(4):
        for seq in range(seqs):
            raw_split[seq, matrix * slots : (matrix + 1) * slots, :] = raw[
                seq * slots : (seq + 1) * slots, matrix * own_cols : (matrix + 1) * own_cols
            ]
    swap_src[...] = raw_split[...].astype(BF16)
    for other, device in far_columns:
        column = device["kv"]
        send(swap_src.at[column], swap_dst.at[kv], send_swap.at[column], recv_swap.at[kv], device)
    swap_dst[pl.ds(kv, 1)] = swap_src[pl.ds(kv, 1)]
    for other, device in near_columns:
        column = device["kv"]
        arrived(
            swap_src.at[column],
            swap_dst.at[column],
            send_swap.at[column],
            recv_swap.at[column],
            device,
        )

    lane = lax.broadcasted_iota(jnp.int32, (4 * slots, chans), 1) // sub
    arrivals = [swap_dst[part].astype(F32) for part in range(kv_size)]
    for head in range(heads):
        tile, spot = divmod(head, per_tile)
        joined = None
        for part in range(kv_size):
            piece_of = arrivals[part][:, tile * chans : (tile + 1) * chans]
            shift = ((part - spot) * sub) % chans
            turned = pltpu.roll(piece_of, shift, 1) if shift else piece_of
            joined = turned if joined is None else jnp.where(lane == part, turned, joined)
        by_slot[:, head, :] = joined

    length = lengths_s[kv]
    lower = lower_v[...]
    queries, forgets, writes, values, gates = [], [], [], [], []
    for slot in range(slots):
        alive = slot < length
        query_raw = by_slot[slot]
        gate_raw = by_slot[3 * slots + slot]
        queries.append(query_raw * jax.nn.sigmoid(query_raw))
        gates.append(gate_raw * jax.nn.sigmoid(gate_raw))
        forget = lower + (1.0 - lower) * jax.nn.sigmoid(by_slot[slots + slot])
        forgets.append(jnp.where(alive, forget, 1.0))
        writes.append(jnp.where(alive, 1.0 - forget, 0.0))
        values.append(by_slot[2 * slots + slot])
    decayed, total = [], None
    for slot in range(slots):
        total = forgets[slot] if total is None else total * forgets[slot]
        decayed.append(queries[slot] * total)
    stacked = jnp.concatenate(decayed, axis=0)
    row_head = lax.broadcasted_iota(jnp.int32, (slots * heads, chans), 0) % heads
    spread = jnp.concatenate(
        [jnp.where(row_head == head, stacked, 0.0).astype(BF16) for head in range(heads)], axis=1
    )
    from_state = jnp.dot(spread, state_half, preferred_element_type=F32)
    kept = list(writes)
    for slot in range(slots):
        for earlier in range(slot):
            kept[earlier] = kept[earlier] * forgets[slot]
        readout = from_state[slot * heads : (slot + 1) * heads]
        for earlier in range(slot + 1):
            weight = jnp.sum(queries[slot] * kept[earlier], axis=-1, keepdims=True)
            readout = readout + weight * values[earlier]
        readout = jnp.where(slot < length, readout, 0.0)
        scaled = readout * lax.rsqrt(jnp.mean(readout * readout, axis=-1, keepdims=True) + 1e-06)
        mix_rows[slot] = scaled * head_v[...] * gates[slot]
    for head in range(heads):
        mix_src[:, head * chans : (head + 1) * chans] = mix_rows[:, head, :].astype(BF16)
    for other, device in far_peers:
        send(mix_src, mix_dst.at[me], send_mix.at[other], recv_mix.at[me], device)

    columns = jnp.concatenate([total] + kept, axis=0).T
    for head in range(heads):
        fresh = columns[:, head : head + 1] * state_v[head]
        for slot in range(slots):
            at = (slot + 1) * heads + head
            fresh = fresh + columns[:, at : at + 1] * values[slot][head : head + 1]
        new_state[head] = fresh

    loads[9].wait()
    arrived(w_out.at[:, mate_out], w_out_v.at[mate], send_out.at[0], recv_out.at[0], mate_device)
    mix_dst[pl.ds(me, 1)] = mix_src[...][None]
    for other, device in near_peers:
        arrived(mix_src, mix_dst.at[other], send_mix.at[other], recv_mix.at[other], device)
    for column in range(kv_size):
        for core in range(tp_size):
            mix_wide[core, column * slots : (column + 1) * slots, :] = mix_dst[
                column * tp_size + core
            ].astype(F32)
    middle = own_tok
    for core in range(tp_size):
        middle = middle + jnp.dot(
            mix_wide[core].astype(BF16), w_out_v[core], preferred_element_type=F32
        )
    mid_src[...] = middle.astype(BF16)
    for other, device in far_peers:
        send(mid_src, mid_dst.at[me], send_mid.at[other], recv_mid.at[me], device)

    loads[10].wait()
    loads[11].wait()
    own_mid = mid_src[...].astype(F32)
    squares = folded(own_mid)
    upward = jnp.dot(
        (own_mid * mixer_v[:, span(me)]).astype(BF16),
        w_up_v[span(me), :],
        preferred_element_type=F32,
    )
    for other, device in near_peers:
        arrived(mid_src, mid_dst.at[other], send_mid.at[other], recv_mid.at[other], device)
        block = mid_dst[other].astype(F32)
        squares = squares + folded(block)
        upward = upward + jnp.dot(
            (block * mixer_v[:, span(other)]).astype(BF16),
            w_up_v[span(other), :],
            preferred_element_type=F32,
        )
    upward = upward * lax.rsqrt(jnp.sum(squares, axis=-1, keepdims=True) / width + 1e-06)
    activated = jnp.square(jnp.maximum(upward, 0.0)).astype(BF16)
    loads[12].wait()

    def down_piece(other):
        return jnp.dot(activated, w_down_v[:, span(other)], preferred_element_type=F32)

    for other, device in far_peers:
        red_src[other] = down_piece(other).astype(BF16)
        send(red_src.at[other], red_dst.at[me], send_red.at[other], recv_red.at[me], device)
    done = own_mid + down_piece(me)
    for other, device in near_peers:
        arrived(red_src.at[other], red_dst.at[other], send_red.at[other], recv_red.at[other], device)
        done = done + red_dst[other].astype(F32)
    slot_of = lax.broadcasted_iota(jnp.int32, (slots, piece), 0)
    for seq in range(seqs):
        kept_rows = jnp.where(
            slot_of < lengths_s[seq], done[seq * slots : (seq + 1) * slots], 0.0
        )
        result[seq] = kept_rows.astype(BF16)
    for copy in sent:
        copy.wait_send()


def store_kernel(result, new_state, result_out, state_out, store_sem):
    heads = new_state.shape[0]
    parts = 4 if heads % 4 == 0 else 1
    chunk = heads // parts
    copies = [pltpu.make_async_copy(result, result_out, store_sem.at[parts])]
    for part in range(parts):
        own = pl.ds(part * chunk, chunk)
        copies.append(
            pltpu.make_async_copy(new_state.at[own], state_out.at[own], store_sem.at[part])
        )
    for copy in copies:
        copy.start()
    for copy in copies:
        copy.wait()


def local_kernel(
    tokens,
    lengths,
    carried,
    norm_mix,
    w_query,
    w_forget,
    w_input,
    w_gate,
    lower_bound,
    head_gain,
    w_out,
    mixer_norm_gain,
    w_up,
    w_down,
):
    kv_size = lax.axis_size("kv")
    tp_size = lax.axis_size("tp")
    group = kv_size * tp_size
    seqs, slots, piece = tokens.shape
    _, heads, chans, _ = carried.shape
    model, _, sub = w_query.shape
    rows, pair, cols = seqs * slots, piece * tp_size, heads * sub
    hidden = w_up.shape[1]

    def turned(weight):
        return weight.transpose(1, 2, 0).reshape(cols, model)

    anywhere = pl.BlockSpec(memory_space=pl.ANY)
    inside = pl.BlockSpec(memory_space=pltpu.VMEM)
    outside = pl.BlockSpec(memory_space=pltpu.HBM)
    dma = pltpu.SemaphoreType.DMA
    vmem = pltpu.VMEM
    result, new_state = pl.pallas_call(
        functools.partial(step_kernel, kv_size, tp_size),
        out_shape=(
            vmem(tokens.shape, BF16),
            vmem((heads, chans, chans), F32),
        ),
        in_specs=[outside] * 14,
        out_specs=(inside, inside),
        scratch_shapes=[
            vmem((seqs, slots, piece), BF16),
            vmem((group, seqs, slots, piece), BF16),
            pltpu.SMEM((seqs,), jnp.int32),
            vmem((heads, chans, chans), F32),
            vmem((1, model), F32),
            vmem((4, cols, model), BF16),
            vmem((model, 4 * cols), BF16),
            vmem((heads, chans), F32),
            vmem((1, chans), F32),
            vmem((tp_size, heads * chans, piece), BF16),
            vmem((1, model), F32),
            vmem((model, hidden), BF16),
            vmem((hidden, model), BF16),
            vmem((seqs, 4 * slots, cols), F32),
            vmem((seqs, 4 * slots, cols), BF16),
            vmem((kv_size, 4 * slots, cols), BF16),
            vmem((4 * slots, heads, chans), F32),
            vmem((slots, heads, chans), F32),
            vmem((slots, heads * chans), BF16),
            vmem((group, slots, heads * chans), BF16),
            vmem((tp_size, rows, heads * chans), F32),
            vmem((rows, piece), BF16),
            vmem((group, rows, piece), BF16),
            vmem((group, rows, piece), BF16),
            vmem((group, rows, piece), BF16),
            dma((14,)),
            dma((group,)),
            dma((group,)),
            dma((1,)),
            dma((1,)),
            dma((kv_size,)),
            dma((kv_size,)),
            dma((group,)),
            dma((group,)),
            dma((group,)),
            dma((group,)),
            dma((group,)),
            dma((group,)),
        ],
        compiler_params=pltpu.CompilerParams(
            collective_id=0, has_side_effects=True, vmem_limit_bytes=56000 * 1024
        ),
    )(
        tokens,
        lengths,
        carried.reshape(heads, chans, chans),
        norm_mix.reshape(1, model),
        turned(w_query),
        turned(w_forget),
        turned(w_input),
        turned(w_gate),
        lower_bound,
        head_gain.reshape(1, chans),
        w_out.reshape(heads * chans, pair),
        mixer_norm_gain.reshape(1, model),
        w_up,
        w_down,
    )
    result, new_state = pl.pallas_call(
        store_kernel,
        out_shape=(
            jax.ShapeDtypeStruct(tokens.shape, BF16),
            jax.ShapeDtypeStruct((heads, chans, chans), F32),
        ),
        in_specs=[inside] * 2,
        out_specs=(anywhere, anywhere),
        scratch_shapes=[dma((5,))],
        compiler_params=pltpu.CompilerParams(vmem_limit_bytes=4000 * 1024),
    )(result, new_state)
    return result, new_state.reshape(carried.shape)


def local(*arrays):
    tokens, carried, weight = arrays[0], arrays[2], arrays[4]
    aligned = (
        tokens.shape[2] % 128 == 0
        and carried.shape[0] == 1
        and carried.shape[2] % 128 == 0
        and carried.shape[2] % weight.shape[2] == 0
        and (weight.shape[1] * weight.shape[2]) % carried.shape[2] == 0
        and lax.axis_size("tp") == 2
        and tokens.shape[1] % 4 == 0
    )
    return (local_kernel if aligned else local_collectives)(*arrays)


def solution(mesh):
    placed = (
        P("dp", None, ("kv", "tp")),
        P("dp"),
        P(("dp", "kv"), "tp", None, None),
        P(),
        P(None, "tp", "kv"),
        P(None, "tp", "kv"),
        P(None, "tp", "kv"),
        P(None, "tp", "kv"),
        P("tp", None),
        P(),
        P("tp", None, "kv"),
        P(),
        P(None, ("kv", "tp")),
        P(("kv", "tp"), None),
    )
    return jax.shard_map(
        local,
        mesh=mesh,
        in_specs=placed,
        out_specs=(P("dp", None, ("kv", "tp")), P(("dp", "kv"), "tp", None, None)),
        check_vma=False,
    )
```

```python
import functools

import jax
import jax.numpy as jnp
from jax import lax
from jax.experimental import pallas as pl
from jax.experimental.pallas import tpu as pltpu
from jax.sharding import PartitionSpec as P


def norm_rows(values, gain):
    floated = values.astype(jnp.float32)
    scaled = floated * lax.rsqrt(jnp.mean(floated * floated, axis=-1, keepdims=True) + 1e-06)
    return (scaled * gain).astype(jnp.bfloat16)


def local_collectives(
    tokens,
    lengths,
    carried,
    norm_mix,
    w_query,
    w_forget,
    w_input,
    w_gate,
    lower_bound,
    head_gain,
    w_out,
    mixer_norm_gain,
    w_up,
    w_down,
):
    tp_size = lax.axis_size("tp")
    seq_group, new_rows, piece_width = tokens.shape
    seq_dev = carried.shape[0]
    gathered = lax.all_gather(tokens, ("kv", "tp"), axis=2, tiled=True)
    normed = norm_rows(gathered, norm_mix)
    model_width = gathered.shape[2]

    def project(weight):
        return jnp.einsum(
            "snd,dhk->snhk", normed, weight, preferred_element_type=jnp.float32
        ).astype(jnp.bfloat16)

    query_raw, forget_raw, value_raw, gate_raw = (
        lax.all_to_all(project(w_query), "kv", split_axis=0, concat_axis=3, tiled=True),
        lax.all_to_all(project(w_forget), "kv", split_axis=0, concat_axis=3, tiled=True),
        lax.all_to_all(project(w_input), "kv", split_axis=0, concat_axis=3, tiled=True),
        lax.all_to_all(project(w_gate), "kv", split_axis=0, concat_axis=3, tiled=True),
    )
    own_lengths = lax.dynamic_slice_in_dim(lengths, lax.axis_index("kv") * seq_dev, seq_dev)
    query_vector = jax.nn.silu(query_raw.astype(jnp.float32))
    forget = lower_bound + (1.0 - lower_bound) * jax.nn.sigmoid(forget_raw.astype(jnp.float32))
    written = 1.0 - forget
    values = value_raw.astype(jnp.float32)
    outer_state = carried
    readouts = []
    for token_position in range(new_rows):
        alive = (token_position < own_lengths)[:, None, None, None]
        updated = (
            forget[:, token_position, :, :, None] * outer_state
            + written[:, token_position, :, :, None] * values[:, token_position, :, None, :]
        )
        outer_state = jnp.where(alive, updated, outer_state)
        state_readout = jnp.einsum(
            "shk,shkv->shv",
            query_vector[:, token_position],
            outer_state,
            precision=lax.Precision.HIGHEST,
        )
        readouts.append(jnp.where(alive[..., 0], state_readout, jnp.float32(0.0)))
    state_readout = jnp.stack(readouts, axis=1)
    scaled = state_readout * lax.rsqrt(
        jnp.mean(state_readout * state_readout, axis=-1, keepdims=True) + 1e-06
    )
    mixed = (scaled * head_gain * jax.nn.silu(gate_raw.astype(jnp.float32))).astype(jnp.bfloat16)
    branch = jnp.einsum(
        "snhv,hvd->snd",
        lax.all_gather(mixed, "kv", axis=0, tiled=True),
        w_out,
        preferred_element_type=jnp.float32,
    )
    pair_width = piece_width * tp_size
    summed_total = lax.psum(branch, "tp")
    pair_cols = lax.dynamic_slice_in_dim(gathered, lax.axis_index("kv") * pair_width, pair_width, 2)
    pair_mid = (pair_cols.astype(jnp.float32) + summed_total).astype(jnp.bfloat16)
    full_pair = lax.all_gather(pair_mid, "kv", axis=2, tiled=True)
    middle = lax.dynamic_slice_in_dim(pair_mid, lax.axis_index("tp") * piece_width, piece_width, 2)
    hidden_in = norm_rows(full_pair, mixer_norm_gain).reshape(seq_group * new_rows, model_width)
    upward = jnp.dot(hidden_in, w_up, preferred_element_type=jnp.float32)
    activated = jnp.square(jax.nn.relu(upward)).astype(jnp.bfloat16)
    collected = lax.psum_scatter(
        jnp.einsum("fd,rf->dr", w_down, activated, preferred_element_type=jnp.float32),
        ("kv", "tp"),
        scatter_dimension=0,
        tiled=True,
    )
    down_part = collected.T.reshape(seq_group, new_rows, piece_width)
    alive_rows = (jnp.arange(new_rows)[None, :] < lengths[:, None])[:, :, None]
    result = jnp.where(alive_rows, middle.astype(jnp.float32) + down_part, jnp.float32(0.0)).astype(
        jnp.bfloat16
    )
    return (result, outer_state)


MESH = pl.DeviceIdType.MESH
F32 = jnp.float32
BF16 = jnp.bfloat16


def step_kernel(
    kv_size,
    tp_size,
    tokens,
    lengths,
    carried,
    norm_mix,
    w_query,
    w_forget,
    w_input,
    w_gate,
    lower_bound,
    head_gain,
    w_out,
    mixer_gain,
    w_up,
    w_down,
    result,
    new_state,
    tok_own,
    tok_all,
    lengths_s,
    state_v,
    norm_v,
    w_proj,
    w_turned,
    lower_v,
    head_v,
    w_out_v,
    mixer_v,
    w_up_v,
    w_down_v,
    raw_split,
    scale_v,
    swap_src,
    swap_dst,
    by_slot,
    mix_rows,
    mix_src,
    mix_dst,
    mix_wide,
    mid_src,
    mid_dst,
    red_src,
    red_dst,
    load_sem,
    entered,
    send_sem,
    recv_out,
    recv_swap,
    recv_wide,
    recv_near,
):
    seqs, slots, piece = tok_own.shape
    group = kv_size * tp_size
    heads, chans = lower_v.shape
    width = group * piece
    pair = tp_size * piece
    own_cols = w_proj.shape[1]
    sub = own_cols // heads
    per_tile = chans // sub
    kv = lax.axis_index("kv")
    tp = lax.axis_index("tp")
    me = kv * tp_size + tp
    mate = tp_size - 1 - tp

    token_load = pltpu.make_async_copy(tokens, tok_own, load_sem.at[0])
    token_load.start()

    mirrored = [kv, kv + 1 - 2 * lax.rem(kv, 2), lax.rem(kv + 2, 4), 3 - kv]

    def along(step):
        return mirrored[step] if kv_size == 4 else lax.rem(kv + step, kv_size)

    near_columns = [along(hop) for hop in range(1, kv_size)]
    far_columns = near_columns[::-1]
    mate_device = {"kv": kv, "tp": mate}

    def cores(column):
        return [{"kv": column, "tp": core} for core in range(tp_size)]

    barrier = pltpu.get_barrier_semaphore()
    pl.semaphore_signal(barrier, inc=1, device_id=mate_device, device_id_type=MESH)
    for column in near_columns:

        @pl.when(column > kv)
        def _():
            for device in cores(column):
                pl.semaphore_signal(barrier, inc=1, device_id=device, device_id_type=MESH)

    own_out = pl.ds(pl.multiple_of(tp * piece, piece), piece)
    mate_out = pl.ds(pl.multiple_of(mate * piece, piece), piece)
    matrix_loads = [
        pltpu.make_async_copy(weight, w_proj.at[at], load_sem.at[1 + at])
        for at, weight in enumerate((w_query, w_forget, w_input, w_gate))
    ]
    small_loads = [
        pltpu.make_async_copy(norm_mix, norm_v, load_sem.at[5]),
        pltpu.make_async_copy(lower_bound, lower_v, load_sem.at[6]),
        pltpu.make_async_copy(head_gain, head_v, load_sem.at[7]),
        pltpu.make_async_copy(lengths, lengths_s, load_sem.at[8]),
    ]
    state_load = pltpu.make_async_copy(carried, state_v, load_sem.at[1])
    out_load = pltpu.make_async_copy(w_out.at[:, own_out], w_out_v.at[tp], load_sem.at[2])
    mixer_load = pltpu.make_async_copy(mixer_gain, mixer_v, load_sem.at[3])
    up_load = pltpu.make_async_copy(w_up, w_up_v, load_sem.at[4])
    down_load = pltpu.make_async_copy(w_down, w_down_v, load_sem.at[0])
    for copy in matrix_loads + small_loads:
        copy.start()

    def remote(src, dst, phase, recv_sem, device):
        return pltpu.make_async_remote_copy(
            src_ref=src,
            dst_ref=dst,
            send_sem=send_sem.at[phase],
            recv_sem=recv_sem,
            device_id=device,
            device_id_type=MESH,
        )

    def arrived(ref, recv_sem):
        remote(ref, ref, 0, recv_sem, mate_device).wait_recv()

    def duo(column):
        return pl.ds(pl.multiple_of(column * tp_size, tp_size), tp_size)

    def span(part):
        return pl.ds(pl.multiple_of(part * pair, pair), pair)

    def give_tokens(device):
        remote(tok_own, tok_all.at[me], 0, recv_wide.at[kv], device).start()

    pl.semaphore_wait(barrier, tp_size * kv + tp_size - 1)
    for column in far_columns:

        @pl.when(column < kv)
        def _():
            for device in cores(column):
                pl.semaphore_signal(
                    entered.at[kv], inc=1, device_id=device, device_id_type=MESH
                )

    token_load.wait()
    for column in far_columns:

        @pl.when(column < kv)
        def _():
            for device in cores(column):
                give_tokens(device)

    give_tokens(mate_device)
    tok_all[pl.ds(me, 1)] = tok_own[...][None]
    later = [state_load, out_load, mixer_load, up_load]
    for matrix in range(4):
        matrix_loads[matrix].wait()
        later[matrix].start()
        w_turned[:, matrix * own_cols : (matrix + 1) * own_cols] = w_proj[matrix].T
    down_load.start()
    for column in near_columns:

        @pl.when(column > kv)
        def _():
            pl.semaphore_wait(entered.at[column], tp_size)
            for device in cores(column):
                give_tokens(device)

    remote(w_out.at[:, mate_out], w_out_v.at[tp], 1, recv_out.at[0], mate_device).start()
    state_load.wait()
    state_half = state_v[...].reshape(heads * chans, chans).astype(BF16)
    for copy in small_loads:
        copy.wait()

    def folded(values):
        total = None
        for at in range(0, pair, chans):
            part = values[:, at : at + chans]
            total = part * part if total is None else total + part * part
        return total

    def tokens_of(column):
        halves = []
        for core in range(tp_size):
            block = tok_all[column * tp_size + core]
            halves.append(
                jnp.concatenate([block[seq].astype(F32) for seq in range(seqs)], axis=0)
            )
        return jnp.concatenate(halves, axis=1)

    def gained(block, gain, weights, column):
        return jnp.dot(
            (block * gain[:, span(column)]).astype(BF16),
            weights[span(column), :],
            preferred_element_type=F32,
        )

    raw, squares = None, None
    for column in [kv] + near_columns:
        if raw is None:
            arrived(tok_all.at[kv * tp_size + mate], recv_wide.at[kv])
        else:
            arrived(tok_all.at[duo(column)], recv_wide.at[column])
        block = tokens_of(column)
        product = gained(block, norm_v, w_turned, column)
        raw = product if raw is None else raw + product
        squares = folded(block) if squares is None else squares + folded(block)
    for matrix in range(4):
        for seq in range(seqs):
            raw_split[seq, matrix * slots : (matrix + 1) * slots, :] = raw[
                seq * slots : (seq + 1) * slots, matrix * own_cols : (matrix + 1) * own_cols
            ]
    swap_src[...] = raw_split[...].astype(BF16)
    for column in far_columns:
        remote(
            swap_src.at[column],
            swap_dst.at[kv],
            2,
            recv_swap.at[0],
            {"kv": column, "tp": tp},
        ).start()
    swap_dst[pl.ds(kv, 1)] = swap_src[pl.ds(kv, 1)]
    factor = lax.rsqrt(jnp.sum(squares, axis=-1, keepdims=True) / width + 1e-06)
    for seq in range(seqs):
        scale_v[seq] = jnp.broadcast_to(factor[seq * slots : (seq + 1) * slots], (slots, chans))
    own_scale = scale_v[kv]
    length = lengths_s[kv]
    lower = lower_v[...]
    lane = lax.broadcasted_iota(jnp.int32, (4 * slots, chans), 1) // sub
    arrived(swap_dst.at[pl.ds(0, kv_size - 1)], recv_swap.at[0])

    arrivals = [swap_dst[part].astype(F32) for part in range(kv_size)]
    for head in range(heads):
        tile, spot = divmod(head, per_tile)
        joined = None
        for part in range(kv_size):
            piece_of = arrivals[part][:, tile * chans : (tile + 1) * chans]
            shift = ((part - spot) * sub) % chans
            turned = pltpu.roll(piece_of, shift, 1) if shift else piece_of
            joined = turned if joined is None else jnp.where(lane == part, turned, joined)
        by_slot[:, head, :] = joined

    queries, forgets, writes, values, gates = [], [], [], [], []
    for slot in range(slots):
        alive = slot < length
        scale = own_scale[slot : slot + 1]
        query_raw = by_slot[slot] * scale
        gate_raw = by_slot[3 * slots + slot] * scale
        queries.append(query_raw * jax.nn.sigmoid(query_raw))
        gates.append(gate_raw * jax.nn.sigmoid(gate_raw))
        forget = lower + (1.0 - lower) * jax.nn.sigmoid(by_slot[slots + slot] * scale)
        forgets.append(jnp.where(alive, forget, 1.0))
        writes.append(jnp.where(alive, 1.0 - forget, 0.0))
        values.append(by_slot[2 * slots + slot] * scale)
    decayed, total = [], None
    for slot in range(slots):
        total = forgets[slot] if total is None else total * forgets[slot]
        decayed.append(queries[slot] * total)
    stacked = jnp.concatenate(decayed, axis=0)
    row_head = lax.broadcasted_iota(jnp.int32, (slots * heads, chans), 0) % heads
    spread = jnp.concatenate(
        [jnp.where(row_head == head, stacked, 0.0).astype(BF16) for head in range(heads)], axis=1
    )
    from_state = jnp.dot(spread, state_half, preferred_element_type=F32)
    kept = list(writes)
    for slot in range(slots):
        for earlier in range(slot):
            kept[earlier] = kept[earlier] * forgets[slot]
        readout = from_state[slot * heads : (slot + 1) * heads]
        for earlier in range(slot + 1):
            weight = jnp.sum(queries[slot] * kept[earlier], axis=-1, keepdims=True)
            readout = readout + weight * values[earlier]
        readout = jnp.where(slot < length, readout, 0.0)
        scaled = readout * lax.rsqrt(jnp.mean(readout * readout, axis=-1, keepdims=True) + 1e-06)
        mix_rows[slot] = scaled * head_v[...] * gates[slot]
    for head in range(heads):
        mix_src[:, head * chans : (head + 1) * chans] = mix_rows[:, head, :].astype(BF16)
    for column in far_columns:
        for device in cores(column):
            remote(mix_src, mix_dst.at[me], 3, recv_near.at[kv], device).start()
    remote(mix_src, mix_dst.at[me], 3, recv_near.at[kv], mate_device).start()

    columns = jnp.concatenate([total] + kept, axis=0).T
    for head in range(heads):
        fresh = columns[:, head : head + 1] * state_v[head]
        for slot in range(slots):
            at = (slot + 1) * heads + head
            fresh = fresh + columns[:, at : at + 1] * values[slot][head : head + 1]
        new_state[head] = fresh

    out_load.wait()
    mixer_load.wait()
    up_load.wait()
    down_load.wait()
    arrived(w_out_v.at[mate], recv_out.at[0])
    mix_dst[pl.ds(me, 1)] = mix_src[...][None]
    for column in [kv] + near_columns:
        if column is kv:
            arrived(mix_dst.at[kv * tp_size + mate], recv_near.at[kv])
        else:
            arrived(mix_dst.at[duo(column)], recv_near.at[column])
        for core in range(tp_size):
            mix_wide[core, column] = mix_dst[column * tp_size + core].astype(F32)
    middle = jnp.concatenate([tok_own[seq].astype(F32) for seq in range(seqs)], axis=0)
    for core in range(tp_size):
        mixed = jnp.concatenate([mix_wide[core, seq] for seq in range(seqs)], axis=0)
        middle = middle + jnp.dot(mixed.astype(BF16), w_out_v[core], preferred_element_type=F32)
    mid_src[...] = middle.astype(BF16)
    for column in far_columns:
        for device in cores(column):
            remote(mid_src, mid_dst.at[me], 4, recv_wide.at[kv], device).start()
    remote(mid_src, mid_dst.at[me], 4, recv_wide.at[kv], mate_device).start()

    own_mid = mid_src[...].astype(F32)
    mid_dst[pl.ds(me, 1)] = mid_src[...][None]
    upward, squares = None, None
    for column in [kv] + near_columns:
        if upward is None:
            arrived(mid_dst.at[kv * tp_size + mate], recv_wide.at[kv])
        else:
            arrived(mid_dst.at[duo(column)], recv_wide.at[column])
        block = jnp.concatenate(
            [mid_dst[column * tp_size + core].astype(F32) for core in range(tp_size)], axis=1
        )
        product = gained(block, mixer_v, w_up_v, column)
        upward = product if upward is None else upward + product
        squares = folded(block) if squares is None else squares + folded(block)
    activated = jnp.square(jnp.maximum(upward, 0.0)).astype(BF16)
    inverse = lax.rsqrt(jnp.sum(squares, axis=-1, keepdims=True) / width + 1e-06)
    inverse = inverse * inverse

    def down_halves(column):
        both = jnp.dot(activated, w_down_v[:, span(column)], preferred_element_type=F32) * inverse
        return [both[:, core * piece : (core + 1) * piece] for core in range(tp_size)]

    for column in far_columns:
        halves = down_halves(column)
        for core, device in enumerate(cores(column)):
            spot = column * tp_size + core
            red_src[spot] = halves[core].astype(BF16)
            remote(red_src.at[spot], red_dst.at[me], 5, recv_near.at[kv], device).start()
    halves = down_halves(kv)
    for core in range(tp_size):
        red_src[kv * tp_size + core] = halves[core].astype(BF16)
    own_mate = kv * tp_size + mate
    remote(red_src.at[own_mate], red_dst.at[me], 5, recv_near.at[kv], mate_device).start()
    done = halves[0]
    for core in range(1, tp_size):
        done = jnp.where(tp == core, halves[core], done)
    done = own_mid + done
    for column in [kv] + near_columns:
        if column is kv:
            arrived(red_dst.at[own_mate], recv_near.at[kv])
            done = done + red_dst[own_mate].astype(F32)
        else:
            arrived(red_dst.at[duo(column)], recv_near.at[column])
            for core in range(tp_size):
                done = done + red_dst[column * tp_size + core].astype(F32)
    slot_of = lax.broadcasted_iota(jnp.int32, (slots, piece), 0)
    for seq in range(seqs):
        kept_rows = jnp.where(
            slot_of < lengths_s[seq], done[seq * slots : (seq + 1) * slots], 0.0
        )
        result[seq] = kept_rows.astype(BF16)
    others = pl.ds(0, group - 1)
    for phase, ref in (
        (0, tok_all.at[others]),
        (1, w_out_v.at[0]),
        (2, swap_dst.at[pl.ds(0, kv_size - 1)]),
        (3, mix_dst.at[others]),
        (4, mid_dst.at[others]),
        (5, red_dst.at[others]),
    ):
        remote(ref, ref, phase, recv_out.at[0], mate_device).wait_send()


def store_kernel(result, new_state, result_out, state_out, store_sem):
    heads = new_state.shape[0]
    parts = 4 if heads % 4 == 0 else 1
    chunk = heads // parts
    copies = [pltpu.make_async_copy(result, result_out, store_sem.at[parts])]
    for part in range(parts):
        own = pl.ds(part * chunk, chunk)
        copies.append(
            pltpu.make_async_copy(new_state.at[own], state_out.at[own], store_sem.at[part])
        )
    for copy in copies:
        copy.start()
    for copy in copies:
        copy.wait()


def local_kernel(
    tokens,
    lengths,
    carried,
    norm_mix,
    w_query,
    w_forget,
    w_input,
    w_gate,
    lower_bound,
    head_gain,
    w_out,
    mixer_norm_gain,
    w_up,
    w_down,
):
    kv_size = lax.axis_size("kv")
    tp_size = lax.axis_size("tp")
    group = kv_size * tp_size
    seqs, slots, piece = tokens.shape
    _, heads, chans, _ = carried.shape
    model, _, sub = w_query.shape
    rows, pair, cols = seqs * slots, piece * tp_size, heads * sub
    hidden = w_up.shape[1]

    def turned(weight):
        return weight.transpose(1, 2, 0).reshape(cols, model)

    anywhere = pl.BlockSpec(memory_space=pl.ANY)
    inside = pl.BlockSpec(memory_space=pltpu.VMEM)
    outside = pl.BlockSpec(memory_space=pltpu.HBM)
    dma = pltpu.SemaphoreType.DMA
    vmem = pltpu.VMEM
    result, new_state = pl.pallas_call(
        functools.partial(step_kernel, kv_size, tp_size),
        out_shape=(
            vmem(tokens.shape, BF16),
            vmem((heads, chans, chans), F32),
        ),
        in_specs=[outside] * 14,
        out_specs=(inside, inside),
        scratch_shapes=[
            vmem((seqs, slots, piece), BF16),
            vmem((group, seqs, slots, piece), BF16),
            pltpu.SMEM((seqs,), jnp.int32),
            vmem((heads, chans, chans), F32),
            vmem((1, model), F32),
            vmem((4, cols, model), BF16),
            vmem((model, 4 * cols), BF16),
            vmem((heads, chans), F32),
            vmem((1, chans), F32),
            vmem((tp_size, heads * chans, piece), BF16),
            vmem((1, model), F32),
            vmem((model, hidden), BF16),
            vmem((hidden, model), BF16),
            vmem((seqs, 4 * slots, cols), F32),
            vmem((seqs, slots, chans), F32),
            vmem((seqs, 4 * slots, cols), BF16),
            vmem((kv_size, 4 * slots, cols), BF16),
            vmem((4 * slots, heads, chans), F32),
            vmem((slots, heads, chans), F32),
            vmem((slots, heads * chans), BF16),
            vmem((group, slots, heads * chans), BF16),
            vmem((tp_size, kv_size, slots, heads * chans), F32),
            vmem((rows, piece), BF16),
            vmem((group, rows, piece), BF16),
            vmem((group, rows, piece), BF16),
            vmem((group, rows, piece), BF16),
            dma((9,)),
            pltpu.SemaphoreType.REGULAR((kv_size,)),
            dma((6,)),
            dma((1,)),
            dma((1,)),
            dma((kv_size,)),
            dma((kv_size,)),
        ],
        compiler_params=pltpu.CompilerParams(
            collective_id=0, has_side_effects=True, vmem_limit_bytes=56000 * 1024
        ),
    )(
        tokens,
        lengths,
        carried.reshape(heads, chans, chans),
        norm_mix.reshape(1, model),
        turned(w_query),
        turned(w_forget),
        turned(w_input),
        turned(w_gate),
        lower_bound,
        head_gain.reshape(1, chans),
        w_out.reshape(heads * chans, pair),
        mixer_norm_gain.reshape(1, model),
        w_up,
        w_down,
    )
    result, new_state = pl.pallas_call(
        store_kernel,
        out_shape=(
            jax.ShapeDtypeStruct(tokens.shape, BF16),
            jax.ShapeDtypeStruct((heads, chans, chans), F32),
        ),
        in_specs=[inside] * 2,
        out_specs=(anywhere, anywhere),
        scratch_shapes=[dma((5,))],
        compiler_params=pltpu.CompilerParams(vmem_limit_bytes=4000 * 1024),
    )(result, new_state)
    return result, new_state.reshape(carried.shape)


def local(*arrays):
    tokens, carried, weight = arrays[0], arrays[2], arrays[4]
    aligned = (
        tokens.shape[2] % 128 == 0
        and carried.shape[0] == 1
        and carried.shape[2] % 128 == 0
        and carried.shape[2] % weight.shape[2] == 0
        and (weight.shape[1] * weight.shape[2]) % carried.shape[2] == 0
        and lax.axis_size("tp") == 2
        and tokens.shape[1] % 4 == 0
    )
    return (local_kernel if aligned else local_collectives)(*arrays)


def solution(mesh):
    placed = (
        P("dp", None, ("kv", "tp")),
        P("dp"),
        P(("dp", "kv"), "tp", None, None),
        P(),
        P(None, "tp", "kv"),
        P(None, "tp", "kv"),
        P(None, "tp", "kv"),
        P(None, "tp", "kv"),
        P("tp", None),
        P(),
        P("tp", None, "kv"),
        P(),
        P(None, ("kv", "tp")),
        P(("kv", "tp"), None),
    )
    return jax.shard_map(
        local,
        mesh=mesh,
        in_specs=placed,
        out_specs=(P("dp", None, ("kv", "tp")), P(("dp", "kv"), "tp", None, None)),
        check_vma=False,
    )
```
